32 devices in a mesh: ep: 8 (over z, y), tp: 4 (over x, core).
Axes of the slice: x: 2, y: 2, z: 4, core: 2. Of those that a mesh axis runs over, the one named last changes fastest.
Arguments:
- queries: bfloat16 [2048, 768], P('ep', 'tp'), may hold values from -270 to 270
- key_rows: bfloat16 [2048, 256], P('ep', 'tp'), may hold values from -6 to 6
- value_rows: bfloat16 [2048, 256], P('ep', 'tp'), may hold values from -6 to 6
- sink_logits: float32 [12], P('tp'), may hold values from 2 to 6
- out_weight: bfloat16 [768, 2048], P('tp'), may hold values from -0.21875 to 0.21875
- mix_gain: float32 [2048], replicated, may hold values from 0.1 to 1.9
- moe_tokens: bfloat16 [4096, 2048], P(('ep', 'tp')), may hold values from -600 to 600
- moe_gain: float32 [2048], replicated, may hold values from 0.1 to 1.9
- routes: int32 [4096, 2], P(('ep', 'tp')), may hold values from 0 to 7, all different within a row; in each aligned block of 128 rows (0 to 127, 128 to 255, ...) at most 40 rows name the same one
- route_weights: float32 [4096, 2], P(('ep', 'tp')), may hold values from 0.25 to 1.5
- expert_gate: bfloat16 [8, 2048, 3584], P('ep', None, 'tp'), may hold values from -0.125 to 0.125
- expert_up: bfloat16 [8, 2048, 3584], P('ep', None, 'tp'), may hold values from -0.125 to 0.125
- expert_down: bfloat16 [8, 3584, 2048], P('ep', 'tp'), may hold values from -0.09375 to 0.09375
Outputs:
- mixed: bfloat16 [2048, 2048], P(('ep', 'tp'))
- moe_out: bfloat16 [4096, 2048], P(('ep', 'tp'))
The draws below stay inside these ranges and needn't reach their ends.
Inputs may be any that keep to these rules, and one draw needn't show every extreme that they name: `routes`: each row names 2 different experts. In the rows of one device no expert is named more than 40 times, and in every draw some device names some expert exactly 40 times.
All inputs are finite; a program needn't handle non-finite values.
Results may differ from the reference program's by a relative error of at most 0.012.
Values may be sent and summed in bfloat16 or wider, within the bound.
No kernel may reach another device: no remote copies, remote signals or barrier semaphores. Data moves between devices by JAX's collectives and lax.ppermute only.
A program may use at most 128 MiB of HBM per device.

```python
import math
import jax
import jax.numpy as jnp
import numpy as np
from jax import lax

D = 2048
FF = 3584
HEADS = 12
KV_HEADS = 4
HDIM = 64
GROUP = 3
WINDOW = 128
TOP = 2
TOK_EP = 256
ROWS_DEV = 128
TOKENS = 2048
ROWS = 4096
EXPERTS = 8
CAP = 40
N_EP = 8
N_TP = 4


def attention_draws(key):
    base = jax.random.fold_in(key, 4242)
    key_part = jnp.clip(jax.random.normal(jax.random.fold_in(base, 1), (TOKENS, KV_HEADS, HDIM), jnp.float32), -6.0, 6.0)
    query_part = jnp.clip(jax.random.normal(jax.random.fold_in(base, 2), (TOKENS, KV_HEADS, GROUP, HDIM), jnp.float32), -6.0, 6.0)
    return (key_part, query_part)


def draw_queries(key, part):
    key_part, query_part = attention_draws(key)
    return query_part.reshape(TOKENS, HEADS * HDIM).astype(jnp.bfloat16)


def draw_key_rows(key, part):
    key_part, query_part = attention_draws(key)
    return key_part.reshape(TOKENS, KV_HEADS * HDIM).astype(jnp.bfloat16)


def draw_moe_tokens(key, part):
    base = jax.random.fold_in(key, 5151)
    tokens_draw = jnp.clip(jax.random.normal(jax.random.fold_in(base, 1), (ROWS, D), jnp.float32), -6.0, 6.0)
    return tokens_draw.astype(jnp.bfloat16)


def block_scale(own_key, shape, shards, least, high):
    def one(dim, shards_of):
        draws = jax.random.uniform(jax.random.fold_in(jax.random.fold_in(own_key, 6), dim), (shards_of,), jnp.float32, least / len(shards), high / len(shards))
        return jnp.repeat(jnp.exp(draws), shape[dim] // shards_of).reshape((-1,) + (1,) * (len(shape) - dim - 1))

    loudness = one(*shards[0])
    for cut in shards[1:]:
        loudness = loudness * one(*cut)
    return loudness


def assign_block(stream_key, own, number, rows, count, top, bound, skew):
    sequence = jax.random.permutation(stream_key, count)
    heavy_load, common = load_shares(count, rows * top, bound, skew, True), load_shares(count, rows * top, bound, skew, False)
    places = jnp.arange(count)

    def named(lengths, turn):
        used = int((lengths > 0).sum())
        fixed = max(1, used // 4)
        moved = fixed + (places - fixed + turn * (used - fixed)) % max(1, count - fixed)
        return jnp.zeros((count,), jnp.int32).at[sequence[jnp.where(places < fixed, places, moved)]].set(jnp.asarray(lengths, jnp.int32))

    lengths = jnp.where(number % 4 == 0, named(heavy_load, number // 4), named(common, number - number // 4 - 1))
    mixed = jax.random.permutation(jax.random.fold_in(own, 3), count)
    source_of, receiver = mixed[0:count // 2 * 2:2], mixed[1:count // 2 * 2:2]
    margin = jnp.minimum(lengths[source_of] - 1, bound - lengths[receiver]) // 2
    margin = jnp.where((source_of == sequence[0]) | (receiver == sequence[0]) | (lengths[receiver] == 0), 0, jnp.maximum(margin, 0))
    moved = jax.random.randint(jax.random.fold_in(own, 4), (count // 2,), 0, 1 << 20) % (margin + 1)
    lengths = lengths.at[source_of].add(-moved).at[receiver].add(moved)
    items = jnp.searchsorted(jnp.cumsum(lengths), jnp.arange(rows * top), side="right").astype(jnp.int32)
    grid = items.reshape(top, rows).T
    grid = grid[jax.random.permutation(jax.random.fold_in(own, 1), rows)]
    turn = jax.random.randint(jax.random.fold_in(own, 2), (rows, 1), 0, top)
    return jnp.take_along_axis(grid, (jnp.arange(top)[None, :] + turn) % top, axis=1)


def load_shares(count, total, reach, skew, full):
    portions = [(1 << 20) // math.isqrt(standing ** skew) + 1 for standing in range(1, count + 1)]
    largest = reach if full else min(reach, max(-(-total // count), total * portions[0] // sum(portions)))
    least = 1 if total - largest >= count - 1 else 0
    given, rest = [largest] + [least] * (count - 1), total - largest - least * (count - 1)
    while rest > 0:
        candidates = [i for i in range(1, count) if given[i] < largest] or [i for i in range(1, count) if given[i] < reach]
        mass, remaining = sum([portions[i] for i in candidates]), rest
        for i in candidates:
            extra = min(reach - given[i], max(1, remaining * portions[i] // mass), rest)
            given[i] = given[i] + extra
            rest = rest - extra
    return np.array(given)


def gaussian(stream_key, dims, width, most, cuts=(), held_as=jnp.bfloat16):
    result = jax.random.normal(stream_key, dims, jnp.float32) * width
    if len(cuts) > 0:
        result = block_scale(stream_key, dims, cuts, -0.22, 0.18) * result
    return jnp.clip(result, min=-most, max=most).astype(held_as)


def setup_inputs(seed: int = 0) -> dict:
    arg_keys = jax.random.split(jax.random.key(seed), 14)
    queries = draw_queries(jax.random.fold_in(arg_keys[13], 71), 0)
    key_rows = draw_key_rows(jax.random.fold_in(arg_keys[13], 71), 0)
    value_rows = gaussian(arg_keys[2], (TOKENS, KV_HEADS * HDIM), 1.0, 6.0, ((0, 8), (1, 4)))
    sink_logits = jnp.clip(2.0 + 4.0 * jax.random.uniform(arg_keys[3], (HEADS,), jnp.float32) ** block_scale(arg_keys[3], (HEADS,), ((0, 4),), -0.2, 0.2), 2.0, 6.0)
    out_weight = gaussian(arg_keys[4], (HEADS * HDIM, D), (HEADS * HDIM) ** -0.5, 0.21875, ((0, 4),))
    mix_gain = jnp.clip(1.0 + 0.18 * jax.random.normal(arg_keys[5], (D,), jnp.float32), 0.1, 1.9)
    moe_tokens = draw_moe_tokens(jax.random.fold_in(arg_keys[13], 71), 0)
    moe_gain = jnp.clip(1.0 + 0.18 * jax.random.normal(arg_keys[7], (D,), jnp.float32), 0.1, 1.9)
    routes_keys = jax.random.split(jax.random.fold_in(arg_keys[8], 1), ROWS // ROWS_DEV)
    routes_turns = jax.random.permutation(jax.random.fold_in(arg_keys[8], 3), ROWS // ROWS_DEV)
    routes = jax.vmap(lambda own, number: assign_block(jax.random.fold_in(arg_keys[8], 2), own, number, ROWS_DEV, EXPERTS, TOP, CAP, 0))(routes_keys, routes_turns).reshape((ROWS, TOP))
    route_weights = jnp.clip(jnp.exp(math.log(1.5) - 1.7917595 * jax.random.uniform(arg_keys[9], (ROWS, TOP), jnp.float32) ** block_scale(arg_keys[9], (ROWS, TOP), ((0, 32),), -0.2, 0.2)), 0.25, 1.5)
    expert_gate = gaussian(arg_keys[10], (EXPERTS, D, FF), D ** -0.5, 0.125, ((0, 8), (2, 4)))
    expert_up = gaussian(arg_keys[11], (EXPERTS, D, FF), D ** -0.5, 0.125, ((0, 8), (2, 4)))
    expert_down = gaussian(arg_keys[12], (EXPERTS, FF, D), FF ** -0.5, 0.09375, ((0, 8), (1, 4)))
    return dict(queries=queries, key_rows=key_rows, value_rows=value_rows, sink_logits=sink_logits, out_weight=out_weight, mix_gain=mix_gain, moe_tokens=moe_tokens, moe_gain=moe_gain, routes=routes, route_weights=route_weights, expert_gate=expert_gate, expert_up=expert_up, expert_down=expert_down)


norm_eps = 1e-06
masked_value = -1e+30

def rms_scale(rows_in, gain):
    squares = lax.optimization_barrier(jnp.mean(rows_in * rows_in, axis=-1, keepdims=True))
    return rows_in * lax.rsqrt(squares + norm_eps) * gain

def reference(queries, key_rows, value_rows, sink_logits, out_weight, mix_gain, moe_tokens, moe_gain, routes, route_weights, expert_gate, expert_up, expert_down):
    head_cols = KV_HEADS * HDIM
    padded_keys = jnp.concatenate([jnp.zeros((WINDOW, head_cols), jnp.bfloat16), key_rows], axis=0)
    padded_values = jnp.concatenate([jnp.zeros((WINDOW, head_cols), jnp.bfloat16), value_rows], axis=0)

    def attend_block(block_index):
        first_row = (block_index * TOK_EP).astype(jnp.int32)
        block_queries = lax.dynamic_slice_in_dim(queries, first_row, TOK_EP, 0)
        block_keys = lax.dynamic_slice_in_dim(padded_keys, first_row, TOK_EP + WINDOW, 0)
        block_values = lax.dynamic_slice_in_dim(padded_values, first_row, TOK_EP + WINDOW, 0)
        query_pos = first_row + jnp.arange(TOK_EP, dtype=jnp.int32)
        key_pos = first_row - WINDOW + jnp.arange(TOK_EP + WINDOW, dtype=jnp.int32)
        distance = query_pos[:, None] - key_pos[None, :]
        allowed = (distance >= 0) & (distance < WINDOW) & (key_pos >= 0)[None, :]
        grouped = block_queries.reshape(TOK_EP, KV_HEADS, GROUP, HDIM).astype(jnp.float32)
        keys_f = block_keys.reshape(TOK_EP + WINDOW, KV_HEADS, HDIM).astype(jnp.float32)
        values_f = block_values.reshape(TOK_EP + WINDOW, KV_HEADS, HDIM).astype(jnp.float32)
        scores = jnp.einsum('qkgd,jkd->kgqj', grouped, keys_f) * HDIM ** (-0.5)
        logits = jnp.where(allowed, scores, masked_value)
        sink_logit = sink_logits.reshape(KV_HEADS, GROUP)[:, :, None, None]
        top_value = jnp.maximum(lax.optimization_barrier(jnp.max(logits, axis=-1, keepdims=True)), sink_logit)
        exponent = jnp.exp(logits - top_value)
        denominator = lax.optimization_barrier(jnp.sum(exponent, axis=-1, keepdims=True)) + jnp.exp(sink_logit - top_value)
        probs = (exponent / denominator).astype(jnp.bfloat16)
        attended = jnp.einsum('kgqj,jkd->qkgd', probs.astype(jnp.float32), values_f)
        return attended.astype(jnp.bfloat16).reshape(TOK_EP, HEADS * HDIM)
    attended = lax.map(attend_block, jnp.arange(N_EP, dtype=jnp.int32)).reshape(TOKENS, HEADS * HDIM)
    group_cols = HEADS * HDIM // N_TP
    projected = jnp.zeros((TOKENS, D), jnp.float32)
    for group_index in range(N_TP):
        lower = group_index * group_cols
        partial_value = jnp.dot(attended[:, lower:lower + group_cols], out_weight[lower:lower + group_cols], preferred_element_type=jnp.float32).astype(jnp.bfloat16)
        partial_value = lax.optimization_barrier(partial_value)
        projected = projected + partial_value.astype(jnp.float32)
    mixed = rms_scale(projected, mix_gain).astype(jnp.bfloat16)
    normed = rms_scale(moe_tokens.astype(jnp.float32), moe_gain).astype(jnp.bfloat16)
    slot_limit = N_EP * N_TP * CAP
    ff_block = FF // N_TP

    def expert_step(accumulated, inputs):
        gate_weight, up_weight, down_weight, expert_id = inputs
        chosen = routes == expert_id
        token_weight = lax.optimization_barrier(jnp.sum(jnp.where(chosen, route_weights, jnp.zeros_like(route_weights)), axis=1))
        member = jnp.any(chosen, axis=1)
        token_index = jnp.nonzero(member, size=slot_limit, fill_value=0)[0].astype(jnp.int32)
        valid_slot = jnp.arange(slot_limit, dtype=jnp.int32) < jnp.sum(member.astype(jnp.int32))
        slot_rows = normed[token_index]
        gate_value = jnp.dot(slot_rows, gate_weight, preferred_element_type=jnp.float32)
        up_value = jnp.dot(slot_rows, up_weight, preferred_element_type=jnp.float32)
        hidden = (jax.nn.silu(gate_value) * up_value).astype(jnp.bfloat16)
        summed = jnp.zeros((slot_limit, D), jnp.float32)
        for block_index in range(N_TP):
            lower = block_index * ff_block
            partial_value = jnp.dot(hidden[:, lower:lower + ff_block], down_weight[lower:lower + ff_block], preferred_element_type=jnp.float32).astype(jnp.bfloat16)
            partial_value = lax.optimization_barrier(partial_value)
            summed = summed + partial_value.astype(jnp.float32)
        expert_out = lax.optimization_barrier(summed.astype(jnp.bfloat16))
        row_weight = jnp.where(valid_slot, token_weight[token_index], jnp.zeros_like(token_weight[token_index]))
        accumulated = accumulated.at[token_index].add(row_weight[:, None] * expert_out.astype(jnp.float32))
        return (accumulated, None)
    combined, _ = lax.scan(expert_step, jnp.zeros((ROWS, D), jnp.float32), (expert_gate, expert_up, expert_down, jnp.arange(EXPERTS, dtype=jnp.int32)))
    return (mixed, combined.astype(jnp.bfloat16))
```

```python
import jax
import jax.numpy as jnp
from jax import lax
from jax.sharding import PartitionSpec as P

HDIM = 64
WINDOW = 128

PERMUTE_EP = 8

norm_eps = 1e-06
masked_value = -1e30


def shifted(shard, axis, by):
    size = lax.axis_size(axis)
    pairs = [(i, i + by) for i in range(size) if 0 <= i + by < size]
    return lax.ppermute(shard, axis, pairs)


def crossed(shard, axis, bits):
    size = lax.axis_size(axis)
    return lax.ppermute(shard, axis, [(i, i ^ bits) for i in range(size)])


def rms_scale(rows_in, gain):
    squares = jnp.mean(rows_in * rows_in, axis=-1, keepdims=True)
    return rows_in * lax.rsqrt(squares + norm_eps) * gain


def tp_bits():
    size = lax.axis_size("tp")
    bits = []
    while size > 1:
        size //= 2
        bits.append(size)
    return bits


def tp_gather(rows):
    for bit in tp_bits():
        rows = jnp.concatenate([rows, crossed(rows, "tp", bit)], axis=0)
    return rows


def tp_reduce(partial):
    for bit in reversed(tp_bits()):
        half = partial.shape[0] // 2
        other = crossed(partial[half:], "tp", bit)
        total = partial[:half].astype(jnp.float32) + other.astype(jnp.float32)
        partial = total.astype(jnp.bfloat16)
    return partial


def mixer_local(queries, key_rows, value_rows, sink_logits, out_weight):
    tok_rows = queries.shape[0]
    kv_local = key_rows.shape[1] // HDIM
    group_size = queries.shape[1] // key_rows.shape[1]
    both = jnp.concatenate([key_rows, value_rows], axis=1)
    prev = shifted(both[tok_rows - WINDOW :], "ep", 1)
    kv_cols = key_rows.shape[1]
    all_keys = jnp.concatenate([prev[:, :kv_cols], key_rows], axis=0).reshape(
        tok_rows + WINDOW, kv_local, HDIM
    )
    all_values = jnp.concatenate([prev[:, kv_cols:], value_rows], axis=0).reshape(
        tok_rows + WINDOW, kv_local, HDIM
    )
    offset = lax.axis_index("ep") * tok_rows
    query_pos = offset + jnp.arange(tok_rows, dtype=jnp.int32)
    key_pos = offset - WINDOW + jnp.arange(tok_rows + WINDOW, dtype=jnp.int32)
    distance = query_pos[:, None] - key_pos[None, :]
    allowed = (distance >= 0) & (distance < WINDOW) & (key_pos >= 0)[None, :]
    grouped = queries.reshape(tok_rows, kv_local, group_size, HDIM)
    scores = jnp.einsum(
        "qkgd,jkd->kgqj", grouped, all_keys, preferred_element_type=jnp.float32
    ) * HDIM ** (-0.5)
    logits = jnp.where(allowed, scores, masked_value)
    sink_logit = sink_logits.reshape(kv_local, group_size)[:, :, None, None]
    top_value = jnp.maximum(jnp.max(logits, axis=-1, keepdims=True), sink_logit)
    exponent = jnp.exp(logits - top_value)
    denominator = jnp.sum(exponent, axis=-1, keepdims=True) + jnp.exp(sink_logit - top_value)
    probs = (exponent / denominator).astype(jnp.bfloat16)
    attended = jnp.einsum("kgqj,jkd->qkgd", probs, all_values, preferred_element_type=jnp.float32)
    attended = attended.astype(jnp.bfloat16).reshape(tok_rows, -1)
    return jnp.dot(attended, out_weight, preferred_element_type=jnp.float32).astype(jnp.bfloat16)


def mixer_reduce(partial, mix_gain):
    size = lax.axis_size("tp")
    own = lax.axis_index("tp")
    rows = partial.shape[0] // size
    order = [0]
    for bit in tp_bits():
        order = order + [i ^ bit for i in order]
    blocks = [
        lax.dynamic_slice_in_dim(partial, (own ^ distance) * rows, rows, 0) for distance in order
    ]
    projected = tp_reduce_wide(jnp.concatenate(blocks, axis=0))
    return rms_scale(projected, mix_gain).astype(jnp.bfloat16)


def tp_reduce_wide(partial):
    bits = list(reversed(tp_bits()))
    for number, bit in enumerate(bits):
        half = partial.shape[0] // 2
        other = crossed(partial[half:], "tp", bit)
        total = partial[:half].astype(jnp.float32) + other.astype(jnp.float32)
        if number + 1 < len(bits):
            total = total.astype(jnp.bfloat16)
        partial = total
    return partial


def expert(rows, gate_weight, up_weight, down_weight):
    gate_value = jnp.dot(rows, gate_weight, preferred_element_type=jnp.float32)
    up_value = jnp.dot(rows, up_weight, preferred_element_type=jnp.float32)
    hidden = (jax.nn.silu(gate_value) * up_value).astype(jnp.bfloat16)
    return jnp.dot(hidden, down_weight, preferred_element_type=jnp.float32).astype(jnp.bfloat16)


def route_tables(routes, route_weights, experts, capacity, own):
    tok_rows = routes.shape[0]
    named = jnp.arange(experts, dtype=jnp.int32)[:, None, None] ^ own
    chosen = routes.T[None, :, :] == named
    member = jnp.any(chosen, axis=1)
    weight = jnp.sum(jnp.where(chosen, route_weights.T[None, :, :], 0.0), axis=1)
    token = jnp.arange(tok_rows, dtype=jnp.int32)
    before = (token[:, None] < token[None, :]).astype(jnp.bfloat16)
    earlier = jnp.dot(member.astype(jnp.bfloat16), before, preferred_element_type=jnp.float32)
    rank = jnp.where(member, earlier, -1.0).astype(jnp.int32)
    hits = rank[:, None, :] == jnp.arange(capacity, dtype=jnp.int32)[None, :, None]
    select = hits.astype(jnp.bfloat16)
    spread = jnp.where(hits, weight[:, None, :], 0.0)
    high = spread.astype(jnp.bfloat16)
    low = (spread - high.astype(jnp.float32)).astype(jnp.bfloat16)
    return select, high, low


def shards(
    queries,
    key_rows,
    value_rows,
    sink_logits,
    out_weight,
    mix_gain,
    moe_tokens,
    moe_gain,
    routes,
    route_weights,
    expert_gate,
    expert_up,
    expert_down,
):
    tok_rows, width = moe_tokens.shape
    top_count = routes.shape[1]
    experts = lax.axis_size("ep")
    capacity = tok_rows * top_count * 5 // (4 * experts)
    permuted = experts <= PERMUTE_EP
    own = lax.axis_index("ep") if permuted else jnp.int32(0)
    weights = (expert_gate[0], expert_up[0], expert_down[0])

    select, high, low = route_tables(routes, route_weights, experts, capacity, own)
    normed = rms_scale(moe_tokens.astype(jnp.float32), moe_gain).astype(jnp.bfloat16)
    outgoing = jnp.dot(
        select.reshape(experts * capacity, tok_rows), normed, preferred_element_type=jnp.float32
    )
    outgoing = outgoing.astype(jnp.bfloat16).reshape(experts, capacity, width)

    def combine(first, count, rows):
        cut = slice(first, first + count)
        flat = rows.reshape(count * capacity, width)
        total = None
        for part in (high, low):
            term = lax.dot_general(
                part[cut].reshape(count * capacity, tok_rows),
                flat,
                (((0,), (0,)), ((), ())),
                preferred_element_type=jnp.float32,
            )
            total = term if total is None else total + term
        return total

    partial = mixer_local(queries, key_rows, value_rows, sink_logits, out_weight)
    mixed = mixer_reduce(partial, mix_gain)

    if permuted:
        arrived = []
        for k in range(experts // 2):
            side = crossed(outgoing[2 * k + 1], "ep", 1)
            block = jnp.concatenate([outgoing[2 * k], side], axis=0)
            if k:
                block = crossed(block, "ep", 2 * k)
            arrived.append(block)
        combined = None
        for k, block in enumerate(arrived):
            result = tp_reduce(expert(tp_gather(block), *weights))
            if k:
                result = crossed(result, "ep", 2 * k)
            side = crossed(result[capacity:], "ep", 1)
            term = combine(2 * k, 2, jnp.concatenate([result[:capacity], side], axis=0))
            combined = term if combined is None else combined + term
    else:
        block = lax.all_to_all(outgoing, "ep", split_axis=0, concat_axis=0, tiled=True)
        result = tp_reduce(
            expert(tp_gather(block.reshape(experts * capacity, width)), *weights)
        )
        returned = lax.all_to_all(
            result.reshape(experts, capacity, width), "ep", split_axis=0, concat_axis=0, tiled=True
        )
        combined = combine(0, experts, returned)
    return (mixed, combined.astype(jnp.bfloat16))


def solution(mesh):
    return jax.shard_map(
        shards,
        mesh=mesh,
        in_specs=(
            P("ep", "tp"),
            P("ep", "tp"),
            P("ep", "tp"),
            P("tp"),
            P("tp", None),
            P(),
            P(("ep", "tp"), None),
            P(),
            P(("ep", "tp"), None),
            P(("ep", "tp"), None),
            P("ep", None, "tp"),
            P("ep", None, "tp"),
            P("ep", "tp", None),
        ),
        out_specs=(P(("ep", "tp"), None), P(("ep", "tp"), None)),
        check_vma=False,
    )
```
